32 devices in a mesh: dp: 2 (over x), kv: 8 (over z, y), tp: 2 (over core).
Axes of the slice: x: 2, y: 2, z: 4, core: 2. Of those that a mesh axis runs over, the one named last changes fastest.
Arguments:
- tokens: bfloat16 [32, 16, 2048], P('dp', None, ('kv', 'tp')), may hold values from -190 to 190
- gain_in: float32 [2048], P(('kv', 'tp')), may hold values from 0.1 to 1.9
- w_qdown: bfloat16 [2048, 512], P(('kv', 'tp')), may hold values from -0.125 to 0.125
- w_kvdown: bfloat16 [2048, 256], P(('kv', 'tp')), may hold values from -0.125 to 0.125
- w_ropek: bfloat16 [2048, 32], replicated, may hold values from -0.125 to 0.125
- gain_qlat: float32 [512], replicated, may hold values from 0.1 to 1.9
- gain_kvlat: float32 [256], replicated, may hold values from 0.1 to 1.9
- w_qup: bfloat16 [512, 16, 96], P(None, 'tp'), may hold values from -0.25 to 0.25
- gain_q: float32 [96], replicated, may hold values from 0.4 to 20
- w_ukey: bfloat16 [256, 16, 64], P(None, 'tp'), may hold values from -0.75 to 0.75
- w_uval: bfloat16 [256, 16, 128], P(None, 'tp'), may hold values from -0.375 to 0.375
- w_out: bfloat16 [2048, 2048], P('tp', 'kv'), may hold values from -2.5 to 2.5
- gain_out: float32 [2048], P(('kv', 'tp')), may hold values from 0.1 to 1.9
- cache_lat: bfloat16 [32, 2048, 256], P('dp', 'kv'), may hold values from -6 to 6
- cache_rope: bfloat16 [32, 32, 2048], P('dp', None, 'kv'), may hold values from -6 to 6
- parents: int32 [32, 16], P('dp'), may hold values from -1 to 14, as said below
- lengths: int32 [32], P('dp'), may hold values from 1024 to 2016
- accepted: int32 [32], P('dp'), may hold values from 0 to 16
Outputs:
- attn_out: bfloat16 [32, 16, 2048], P('dp', None, ('kv', 'tp'))
- lat_cache_out: bfloat16 [32, 2048, 256], P('dp', 'kv')
- rope_cache_out: bfloat16 [32, 32, 2048], P('dp', None, 'kv')
The draws below stay inside these ranges and needn't reach their ends.
Inputs may be any that keep to these rules, and one draw needn't show every extreme that they name: `parents`: proposal j's parent is -1 (the last accepted token) or a proposal before j. Rows 0 .. lengths + accepted - 1 of a sequence's cache hold its past; the 16 positions after them lie inside the cache.
All inputs are finite; a program needn't handle non-finite values.
Results may differ from the reference program's by a relative error of at most 0.0102.
The reference program's roundings to bfloat16 on the way count: a program that leaves them out, or rounds other values in their place, can miss the bound.
Values may be sent and summed in bfloat16 or wider, within the bound.
A program may use at most 64 MiB of HBM per device.

```python
import jax
import jax.numpy as jnp
from jax import lax

MODEL = 2048
HEADS = 16
QRANK = 512
KVRANK = 256
NOPE = 64
ROPE = 32
VHEAD = 128
PROPS = 16
QKHEAD = 96
SEQS = 32
POSITIONS = 2048


def draw_tokens(key, part):
    base_key, rough_key, row_key = jax.random.split(jax.random.fold_in(key, 11), 3)
    column = jnp.arange(MODEL, dtype=jnp.float32) / (MODEL - 1)
    ramp = jnp.exp(jnp.log(10.0) * column)
    rough = jax.random.uniform(rough_key, (MODEL,), jnp.float32, 0.5, 1.5)
    row_scale = jnp.exp(jax.random.uniform(row_key, (SEQS, PROPS, 1), jnp.float32, 0.0, jnp.log(10.0)))
    noise = jax.random.normal(base_key, (SEQS, PROPS, MODEL), jnp.float32)
    noise = jnp.clip(noise, -5.0, 5.0)
    return (noise * ramp * rough * row_scale / 4.0).astype(jnp.bfloat16)


def draw_gain_q(key, part):
    inner = jax.random.fold_in(key, 23)
    values = 1.0 + 0.18 * jnp.clip(jax.random.normal(inner, (QKHEAD,), jnp.float32), -3.0, 3.0)
    return values.astype(jnp.float32)


def draw_w_out(key, part):
    base_key, rough_key = jax.random.split(jax.random.fold_in(key, 37), 2)
    column = jnp.arange(MODEL, dtype=jnp.float32) / (MODEL - 1)
    ramp = jnp.exp(jnp.log(10.0) * column)
    rough = jax.random.uniform(rough_key, (MODEL,), jnp.float32, 0.5, 1.5)
    noise = jnp.clip(jax.random.normal(base_key, (HEADS * VHEAD, MODEL), jnp.float32), -5.0, 5.0)
    return (noise * ramp * rough / 30.0).astype(jnp.bfloat16)


def draw_parents(key, part):
    raw = jax.random.randint(jax.random.fold_in(key, 41), (SEQS, PROPS), 0, 1 << 20, dtype=jnp.int32)
    limit = jnp.arange(PROPS, dtype=jnp.int32) + 1
    return (raw % limit[None, :] - 1).astype(jnp.int32)


def plant(values, rng, least, high):
    longest = values.shape.index(max(values.shape))
    spots = []
    for shift in (0, 1):
        where = [jax.random.randint(jax.random.fold_in(rng, axis), (), 0, length) for axis, length in enumerate(values.shape)]
        where[longest] = (where[longest] + shift) % values.shape[longest]
        spots.append(tuple(where))
    return values.at[spots[0]].set(least).at[spots[1]].set(high)


def level_of(key, extent, cuts, low, high):
    factor_of, own = 1.0, jax.random.fold_in(key, 6)
    for dim, parts in cuts:
        draws = jnp.exp(jax.random.uniform(jax.random.fold_in(own, dim), (parts,), jnp.float32, low / len(cuts), high / len(cuts)))
        factor_of = factor_of * jnp.repeat(draws, extent[dim] // parts).reshape([-1 if axis == dim else 1 for axis in range(len(extent))])
    return factor_of


def centred(stream_key, shape, scale, most, pieces=(), held_as=jnp.bfloat16):
    level = level_of(stream_key, shape, pieces, -0.22, 0.18) if pieces else 1.0
    entries = jax.random.normal(stream_key, shape, jnp.float32) * scale * level
    return jnp.minimum(jnp.maximum(entries, -most), most).astype(held_as)


def setup_inputs(seed: int = 0) -> dict:
    streams_of = jax.random.split(jax.random.key(seed), 19)
    return {
        "tokens": draw_tokens(jax.random.fold_in(streams_of[18], 71), 0),
        "gain_in": jnp.clip(1.0 + 0.18 * jax.random.normal(streams_of[1], (MODEL,), jnp.float32), 0.1, 1.9),
        "w_qdown": centred(streams_of[2], (MODEL, QRANK), MODEL ** -0.5, 0.125, ((0, 16),)),
        "w_kvdown": centred(streams_of[3], (MODEL, KVRANK), MODEL ** -0.5, 0.125, ((0, 16),)),
        "w_ropek": centred(streams_of[4], (MODEL, ROPE), MODEL ** -0.5, 0.125),
        "gain_qlat": jnp.clip(1.0 + 0.18 * jax.random.normal(streams_of[5], (QRANK,), jnp.float32), 0.1, 1.9),
        "gain_kvlat": jnp.clip(1.0 + 0.18 * jax.random.normal(streams_of[6], (KVRANK,), jnp.float32), 0.1, 1.9),
        "w_qup": centred(streams_of[7], (QRANK, HEADS, QKHEAD), QRANK ** -0.5, 0.25, ((1, 2),)),
        "gain_q": draw_gain_q(jax.random.fold_in(streams_of[18], 71), 0),
        "w_ukey": centred(streams_of[9], (KVRANK, HEADS, NOPE), NOPE ** -0.5, 0.75, ((1, 2),)),
        "w_uval": centred(streams_of[10], (KVRANK, HEADS, VHEAD), KVRANK ** -0.5, 0.375, ((1, 2),)),
        "w_out": draw_w_out(jax.random.fold_in(streams_of[18], 71), 0),
        "gain_out": jnp.clip(1.0 + 0.18 * jax.random.normal(streams_of[12], (MODEL,), jnp.float32), 0.1, 1.9),
        "cache_lat": centred(streams_of[13], (SEQS, POSITIONS, KVRANK), 1.0, 6.0, ((0, 2), (1, 8))),
        "cache_rope": centred(streams_of[14], (SEQS, ROPE, POSITIONS), 1.0, 6.0, ((0, 2), (2, 8))),
        "parents": draw_parents(jax.random.fold_in(streams_of[18], 71), 0),
        "lengths": plant(jax.random.randint(streams_of[16], (SEQS,), POSITIONS // 2, POSITIONS - 2 * PROPS + 1), jax.random.fold_in(streams_of[16], 1), POSITIONS // 2, POSITIONS - 2 * PROPS).astype(jnp.int32),
        "accepted": plant(jax.random.randint(streams_of[17], (SEQS,), 0, PROPS + 1), jax.random.fold_in(streams_of[17], 1), 0, PROPS).astype(jnp.int32),
    }


epsilon = 1e-06

def normed(values, gain_vec):
    return values * lax.rsqrt(lax.optimization_barrier(jnp.mean(values * values, axis=-1, keepdims=True)) + epsilon) * gain_vec

def rope_angles(position, half_dim):
    frequency = 10000.0 ** (-(jnp.arange(half_dim, dtype=jnp.float32) * 2.0) / (2 * half_dim))
    return position.astype(jnp.float32)[..., None] * frequency

def ancestry(parents):
    proposals = parents.shape[-1]
    parent_link = (parents[..., :, None] == jnp.arange(proposals, dtype=jnp.int32)).astype(jnp.float32)
    identity = jnp.broadcast_to(jnp.eye(proposals, dtype=jnp.float32), parent_link.shape)

    def extend(iteration, state_pair):
        reaches, current = state_pair
        current = jnp.einsum('sij,sjk->sik', current, parent_link, precision=lax.Precision.HIGHEST)
        return (reaches + current, current)
    reaches, current = lax.fori_loop(0, proposals - 1, extend, (identity, identity))
    depths = (lax.optimization_barrier(jnp.sum(reaches, axis=-1)) - 1.0).astype(jnp.int32)
    return (reaches, depths)

def to_half(values):
    return lax.optimization_barrier(values.astype(jnp.bfloat16))

def place_rows(cache_row, new_rows, start_at):
    return lax.dynamic_update_slice(cache_row, new_rows, (start_at, start_at * 0))

def place_columns(cache_row, new_rows, start_at):
    return lax.dynamic_update_slice(cache_row, new_rows.T, (start_at * 0, start_at))

def reference(tokens, gain_in, w_qdown, w_kvdown, w_ropek, gain_qlat, gain_kvlat, w_qup, gain_q, w_ukey, w_uval, w_out, gain_out, cache_lat, cache_rope, parents, lengths, accepted):
    tok32 = tokens.astype(jnp.float32)
    scaled = to_half(tok32 * gain_in).astype(jnp.float32)
    squares = lax.optimization_barrier(jnp.sum(tok32 * tok32, axis=-1))
    rescale = lax.rsqrt(squares / MODEL + epsilon)[..., None]

    def project(weight):
        return jnp.einsum('spd,dk->spk', scaled, weight.astype(jnp.float32)) * rescale
    query_latent = to_half(normed(project(w_qdown), gain_qlat))
    new_latent = to_half(normed(project(w_kvdown), gain_kvlat))
    new_rope = to_half(project(w_ropek))
    reaches, depths = ancestry(parents)
    starts = lengths + accepted
    query_pos = starts[:, None] + depths
    half_dim = ROPE // 2
    queries = jnp.einsum('spr,rhd->sphd', query_latent.astype(jnp.float32), w_qup.astype(jnp.float32))
    queries = normed(queries, gain_q)
    query_nope = to_half(queries[..., :NOPE]).astype(jnp.float32)
    angles = rope_angles(query_pos, half_dim)[:, :, None, :]
    lower_half = queries[..., NOPE:NOPE + half_dim]
    upper_half = queries[..., NOPE + half_dim:]
    query_rot = to_half(jnp.concatenate([lower_half * jnp.cos(angles) - upper_half * jnp.sin(angles), upper_half * jnp.cos(angles) + lower_half * jnp.sin(angles)], axis=-1))
    query_lat = to_half(jnp.einsum('sphn,khn->sphk', query_nope, w_ukey.astype(jnp.float32)))
    lat_out = jax.vmap(place_rows)(cache_lat, new_latent, starts)
    rope_out = jax.vmap(place_columns)(cache_rope, new_rope, starts)

    def attend(item):
        lat_query, rot_query, lat_rows, rope_rows, start_at, reach_one, depth_one = item
        slots = jnp.arange(POSITIONS, dtype=jnp.int32)
        offset = slots - start_at
        inside = (offset >= 0) & (offset < PROPS)
        matches = offset[:, None] == jnp.arange(PROPS, dtype=jnp.int32)[None, :]
        key_pos = jnp.where(inside, start_at + lax.optimization_barrier(jnp.sum(jnp.where(matches, depth_one[None, :], 0), axis=-1)), slots)
        ancestor = jnp.einsum('ij,pj->ip', reach_one, matches.astype(jnp.float32), precision=lax.Precision.HIGHEST)
        visible = (offset < 0)[None, :] | (ancestor > 0.5)
        key_angles = rope_angles(key_pos, half_dim).T
        rope32 = rope_rows.astype(jnp.float32)
        key_low = rope32[:half_dim]
        key_high = rope32[half_dim:]
        key_rot = to_half(jnp.concatenate([key_low * jnp.cos(key_angles) - key_high * jnp.sin(key_angles), key_high * jnp.cos(key_angles) + key_low * jnp.sin(key_angles)], axis=0))
        lat32 = lat_rows.astype(jnp.float32)
        scores = (jnp.einsum('ihk,pk->ihp', lat_query.astype(jnp.float32), lat32) + jnp.einsum('ihr,rp->ihp', rot_query.astype(jnp.float32), key_rot.astype(jnp.float32))) * (NOPE + ROPE) ** (-0.5)
        masked = jnp.where(visible[:, None, :], scores, -jnp.inf)
        row_max = lax.optimization_barrier(jnp.max(masked, axis=-1, keepdims=True))
        weights32 = jnp.exp(masked - row_max)
        denominator = lax.optimization_barrier(jnp.sum(weights32, axis=-1))
        weights = to_half(weights32).astype(jnp.float32)
        numerator = jnp.einsum('ihp,pk->ihk', weights, lat32)
        return (numerator, denominator)
    numerators, denominators = lax.map(attend, (query_lat, query_rot, lat_out, rope_out, starts, reaches, depths))
    valued = jnp.einsum('sphk,khv->sphv', numerators, w_uval.astype(jnp.float32), precision=lax.Precision.HIGHEST)
    head_out = to_half(valued / denominators[..., None])
    head_rows = head_out.reshape(head_out.shape[0], PROPS, HEADS * VHEAD).astype(jnp.float32)
    mixed = jnp.einsum('spx,xd->spd', head_rows, w_out.astype(jnp.float32))
    result = normed(mixed, gain_out).astype(jnp.bfloat16)
    return (result, lat_out, rope_out)
```

```python
import functools

import jax
import jax.numpy as jnp
from jax import lax
from jax.experimental import pallas as pl
from jax.experimental.pallas import tpu as pltpu
from jax.sharding import PartitionSpec as P

epsilon = 1e-06


def normed(values, gain_vec):
    return (
        values * lax.rsqrt(jnp.mean(values * values, axis=-1, keepdims=True) + epsilon) * gain_vec
    )


def rope_angles(position, half_dim):
    frequency = 10000.0 ** (-(jnp.arange(half_dim, dtype=jnp.float32) * 2.0) / (2 * half_dim))
    return position.astype(jnp.float32)[..., None] * frequency


def ancestry(parents):
    proposals = parents.shape[-1]
    parent_link = (parents[..., :, None] == jnp.arange(proposals, dtype=jnp.int32)).astype(
        jnp.float32
    )
    identity = jnp.broadcast_to(jnp.eye(proposals, dtype=jnp.float32), parent_link.shape)

    def extend(iteration, state_pair):
        reaches, current = state_pair
        current = jnp.einsum("sij,sjk->sik", current, parent_link, precision=lax.Precision.HIGHEST)
        return (reaches + current, current)

    reaches, current = lax.fori_loop(0, proposals - 1, extend, (identity, identity))
    depths = (jnp.sum(reaches, axis=-1) - 1.0).astype(jnp.int32)
    return (reaches, depths)


def latents(summed, squares, full_width, gain_qlat, gain_kvlat):
    qrank = gain_qlat.shape[0]
    kvrank = gain_kvlat.shape[0]
    scaled_rows = summed * lax.rsqrt(squares / full_width + epsilon)[:, None]
    query_latent = normed(scaled_rows[:, :qrank], gain_qlat).astype(jnp.bfloat16)
    new_latent = normed(scaled_rows[:, qrank : qrank + kvrank], gain_kvlat).astype(jnp.bfloat16)
    new_rope = scaled_rows[:, qrank + kvrank :].astype(jnp.bfloat16)
    return (query_latent, new_latent, new_rope)


def apply_values(numer_rows, value_map):
    return jnp.einsum("...hk,khv->...hv", numer_rows, value_map, precision=lax.Precision.HIGHEST)


MESH = pl.DeviceIdType.MESH


def remote(src, dst, send_sem, recv_sem, kv, tp):
    return pltpu.make_async_remote_copy(
        src_ref=src,
        dst_ref=dst,
        send_sem=send_sem,
        recv_sem=recv_sem,
        device_id={"kv": kv, "tp": tp},
        device_id_type=MESH,
    )


def greet(nkv, ntp, me_kv, me_tp):
    barrier = pltpu.get_barrier_semaphore()
    for step in range(1, nkv * ntp):
        kv = lax.rem(me_kv + step // ntp, nkv)
        tp = lax.rem(me_tp + step % ntp, ntp)
        pl.semaphore_signal(barrier, inc=1, device_id={"kv": kv, "tp": tp}, device_id_type=MESH)
    return barrier


def visit_order(nz):
    return [nz // 2] + [step for step in range(1, nz) if step != nz // 2] + [0]


def latent_kernel(
    nkv,
    tok_ref,
    gin_ref,
    wq_ref,
    wkv_ref,
    wr_ref,
    gq_ref,
    gk_ref,
    qlat_ref,
    nlat_ref,
    nrope_ref,
    wpad,
    part,
    xbuf,
    sbuf,
    ybuf,
    zbuf,
    rbuf,
    gbuf,
    xsems,
    ysend,
    yrecv,
    zsend,
    zrecv,
    gsend,
    grecv,
    ysend2,
    fsend,
):
    ntp, ny = 2, 2
    nz = nkv // ny
    me_kv, me_tp = lax.axis_index("kv"), lax.axis_index("tp")
    me_z, me_y = me_kv // ny, lax.rem(me_kv, ny)
    other = 1 - me_tp
    mate = me_z * ny + (1 - me_y)
    barrier = greet(nkv, ntp, me_kv, me_tp)
    rows, width = tok_ref.shape
    each = rows // (nkv * ntp)
    qr, kr, rd = wq_ref.shape[1], wkv_ref.shape[1], wr_ref.shape[0]
    full = width * nkv * ntp

    tok = tok_ref[...].astype(jnp.float32)
    scaled = (tok * gin_ref[...]).astype(jnp.bfloat16)
    squares = jnp.sum(tok * tok, axis=-1, keepdims=True)
    wpad[...] = jnp.zeros_like(wpad)
    first = pl.multiple_of((me_kv * ntp + me_tp) * width, width)
    wpad[:rd, :] = wr_ref[:, pl.ds(first, width)]
    pq = jnp.dot(scaled, wq_ref[...], preferred_element_type=jnp.float32)
    pk = jnp.dot(scaled, wkv_ref[...], preferred_element_type=jnp.float32)
    pr = lax.dot_general(
        scaled, wpad[...], (((1,), (1,)), ((), ())), preferred_element_type=jnp.float32
    )
    lane = lax.broadcasted_iota(jnp.int32, pr.shape, 1)
    pr = jnp.where(lane == rd, squares, pr)
    for block in range(nkv * ntp):
        kv, tp = block // ntp, block % ntp
        span = slice(block * each, (block + 1) * each)
        part[tp, kv, :, :qr] = pq[span]
        part[tp, kv, :, qr : qr + kr] = pk[span]
        part[tp, kv, :, qr + kr :] = pr[span]

    pl.semaphore_wait(barrier, nkv * ntp - 1)
    swap = remote(part.at[other], xbuf, xsems.at[0], xsems.at[1], me_kv, other)
    swap.start()
    swap.wait()
    small = lax.broadcasted_iota(jnp.int32, (each, 128), 1)
    for kv in range(nkv):
        sbuf[kv] = part[me_tp, kv] + xbuf[kv]
    sends = []
    order = visit_order(nz)

    def to_mate(z):
        return remote(
            sbuf.at[z * ny + 1 - me_y], ybuf.at[z], ysend.at[z], yrecv.at[z], mate, me_tp
        )

    for step in order:
        copy = to_mate(lax.rem(me_z + step, nz))
        copy.start()
        sends.append(copy)
    for step in order:
        z = lax.rem(me_z + step, nz)
        to_mate(z).wait_recv()
        acc = sbuf[z * ny + me_y] + ybuf[z]
        if step:
            zbuf[z] = acc
            copy = remote(
                zbuf.at[z],
                rbuf.at[me_z],
                zsend.at[z],
                zrecv.at[me_z],
                z * ny + me_y,
                me_tp,
            )
            copy.start()
            sends.append(copy)
    for step in range(1, nz):
        z = lax.rem(me_z + step, nz)
        remote(
            zbuf.at[z], rbuf.at[z], zsend.at[z], zrecv.at[z], z * ny + me_y, me_tp
        ).wait_recv()
        acc = acc + rbuf[z]
    ends = acc[:, qr + kr :]
    square = ends[:, rd : rd + 1]
    scale = lax.rsqrt(square / full + epsilon)
    zq = acc[:, :qr] * scale
    zk = acc[:, qr : qr + kr] * scale
    mine = me_kv * ntp + me_tp
    gbuf[mine, :, :qr] = normed(zq, gq_ref[...]).astype(jnp.bfloat16)
    gbuf[mine, :, qr : qr + kr] = normed(zk, gk_ref[...]).astype(jnp.bfloat16)
    gbuf[mine, :, qr + kr :] = (ends * scale).astype(jnp.bfloat16)

    def pass_on(slot, sem, kv, tp):
        return remote(gbuf.at[slot], gbuf.at[slot], sem, grecv.at[slot], kv, tp)

    for step in order[:-1]:
        z = lax.rem(me_z + step, nz)
        copy = pass_on(mine, gsend.at[step], z * ny + me_y, me_tp)
        copy.start()
        sends.append(copy)
    for step in range(nz):
        kv = lax.rem(me_z + step, nz) * ny + me_y
        slot = kv * ntp + me_tp
        if step:
            pass_on(slot, gsend.at[step], kv, me_tp).wait_recv()
        for copy in (
            pass_on(slot, ysend2.at[step], mate, me_tp),
            pass_on(slot, fsend.at[step], me_kv, other),
        ):
            copy.start()
            sends.append(copy)
    for step in range(nz):
        kv = lax.rem(me_z + step, nz) * ny + 1 - me_y
        slot = kv * ntp + me_tp
        pass_on(slot, ysend2.at[step], mate, me_tp).wait_recv()
        copy = pass_on(slot, fsend.at[nz + step], me_kv, other)
        copy.start()
        sends.append(copy)
    for step in range(nkv):
        kv = lax.rem(me_kv + step, nkv)
        slot = kv * ntp + other
        pass_on(slot, fsend.at[step], me_kv, other).wait_recv()
    for copy in sends:
        copy.wait_send()
    for block in range(nkv * ntp):
        span = slice(block * each, (block + 1) * each)
        qlat_ref[span, :] = gbuf[block, :, :qr]
        nlat_ref[span, :] = gbuf[block, :, qr : qr + kr]
        nrope_ref[span, :] = gbuf[block, :, qr + kr : qr + kr + rd]


def gather_latents(nkv, tokens, gain_in, w_qdown, w_kvdown, w_ropek, gain_qlat, gain_kvlat):
    rows = tokens.shape[0]
    each = rows // (nkv * 2)
    qr, kr, rd = w_qdown.shape[1], w_kvdown.shape[1], w_ropek.shape[1]
    nz = nkv // 2
    wide = qr + kr + 128
    vmem = pl.BlockSpec(memory_space=pltpu.VMEM)
    dma = pltpu.SemaphoreType.DMA
    return pl.pallas_call(
        functools.partial(latent_kernel, nkv),
        out_shape=(
            jax.ShapeDtypeStruct((rows, qr), jnp.bfloat16),
            jax.ShapeDtypeStruct((rows, kr), jnp.bfloat16),
            jax.ShapeDtypeStruct((rows, rd), jnp.bfloat16),
        ),
        in_specs=[vmem] * 7,
        out_specs=(vmem, vmem, vmem),
        scratch_shapes=[
            pltpu.VMEM((128, tokens.shape[1]), jnp.bfloat16),
            pltpu.VMEM((2, nkv, each, wide), jnp.float32),
            pltpu.VMEM((nkv, each, wide), jnp.float32),
            pltpu.VMEM((nkv, each, wide), jnp.float32),
            pltpu.VMEM((nz, each, wide), jnp.float32),
            pltpu.VMEM((nz, each, wide), jnp.float32),
            pltpu.VMEM((nz, each, wide), jnp.float32),
            pltpu.VMEM((nkv * 2, each, wide), jnp.bfloat16),
            dma((2,)),
            dma((nz,)),
            dma((nz,)),
            dma((nz,)),
            dma((nz,)),
            dma((nz,)),
            dma((nkv * 2,)),
            dma((nz,)),
            dma((nkv,)),
        ],
        compiler_params=pltpu.CompilerParams(
            collective_id=1, has_side_effects=True, vmem_limit_bytes=48 * 1024 * 1024
        ),
    )(tokens, gain_in[None], w_qdown, w_kvdown, w_ropek.T, gain_qlat[None], gain_kvlat[None])


def output_kernel(
    nkv,
    heads,
    val_ref,
    stat_ref,
    wout_ref,
    gout_ref,
    out_ref,
    ystat,
    mstat,
    zstat,
    scol,
    ybuf,
    zbuf,
    rbuf,
    obuf,
    pbuf,
    xbuf,
    nbuf,
    tsems,
    ysend,
    yrecv,
    tsend,
    trecv,
    zsend,
    zrecv,
    osend,
    orecv,
    fsend,
    xsems,
    nsend,
    nrecv,
):
    ntp, ny = 2, 2
    nz = nkv // ny
    me_kv, me_tp = lax.axis_index("kv"), lax.axis_index("tp")
    me_z, me_y = me_kv // ny, lax.rem(me_kv, ny)
    other = 1 - me_tp
    mate = me_z * ny + (1 - me_y)
    barrier = greet(nkv, ntp, me_kv, me_tp)
    pl.semaphore_wait(barrier, nkv * ntp - 1)
    _, each, channels = val_ref.shape
    vhead = channels // heads
    order = visit_order(nz)
    span = nz * each

    def columns(parts, at):
        stacked = jnp.concatenate(parts, axis=0)
        rest = jnp.zeros((128 - stacked.shape[0], span), jnp.float32)
        turned = jnp.concatenate([stacked, rest], axis=0).T
        for z in range(nz):
            scol[at, z] = turned[z * each : (z + 1) * each]

    def to_mate(z):
        return remote(
            val_ref.at[z * ny + 1 - me_y], ybuf.at[z], ysend.at[z], yrecv.at[z], mate, me_tp
        )

    stat_copy = remote(stat_ref.at[1 - me_y], ystat, tsems.at[0], tsems.at[1], mate, me_tp)
    stat_copy.start()
    sends = []
    for step in order:
        copy = to_mate(lax.rem(me_z + step, nz))
        copy.start()
        sends.append(copy)
    stat_copy.wait()
    here, there = stat_ref[me_y], ystat[...]
    top = jnp.maximum(here[:heads], there[:heads])
    here_scale = jnp.exp(here[:heads] - top)
    there_scale = jnp.exp(there[:heads] - top)
    mstat[:heads] = top
    mstat[heads:] = here[heads:] * here_scale + there[heads:] * there_scale

    def stat_to(step):
        kv = lax.rem(me_z + step, nz) * ny + me_y
        return remote(mstat, zstat.at[me_z], tsend.at[step], trecv.at[me_z], kv, me_tp)

    columns([here_scale, there_scale], 0)
    for step in order[:-1]:
        copy = stat_to(step)
        copy.start()
        sends.append(copy)
    for step in order:
        z = lax.rem(me_z + step, nz)
        to_mate(z).wait_recv()
        factors = scol[0, z]
        acc = []
        for head in range(heads):
            lanes = slice(head * vhead, (head + 1) * vhead)
            term = val_ref[z * ny + me_y, :, lanes].astype(jnp.float32) * factors[
                :, head : head + 1
            ] + ybuf[z, :, lanes].astype(jnp.float32) * factors[
                :, heads + head : heads + head + 1
            ]
            if step:
                zbuf[z, :, lanes] = term.astype(jnp.bfloat16)
            acc.append(term)
        if step:
            copy = remote(
                zbuf.at[z], rbuf.at[me_z], zsend.at[z], zrecv.at[me_z], z * ny + me_y, me_tp
            )
            copy.start()
            sends.append(copy)
    stats = [mstat[...]]
    for step in range(1, nz):
        z = lax.rem(me_z + step, nz)
        remote(
            mstat, zstat.at[z], tsend.at[step], trecv.at[z], z * ny + me_y, me_tp
        ).wait_recv()
        stats.append(zstat[z])
    top = functools.reduce(jnp.maximum, [stat[:heads] for stat in stats])
    scales = [jnp.exp(stat[:heads] - top) for stat in stats]
    total = sum(scale * stat[heads:] for scale, stat in zip(scales, stats))
    columns(scales + [total], 1)
    factors = scol[1, me_z]
    acc = [term * factors[:, head : head + 1] for head, term in enumerate(acc)]
    for step in range(1, nz):
        z = lax.rem(me_z + step, nz)
        remote(
            zbuf.at[z], rbuf.at[z], zsend.at[z], zrecv.at[z], z * ny + me_y, me_tp
        ).wait_recv()
        for head in range(heads):
            at = step * heads + head
            acc[head] = acc[head] + (
                rbuf[z, :, head * vhead : (head + 1) * vhead].astype(jnp.float32)
                * factors[:, at : at + 1]
            )
    for head in range(heads):
        at = nz * heads + head
        obuf[me_kv, :, head * vhead : (head + 1) * vhead] = (
            acc[head] / factors[:, at : at + 1]
        ).astype(jnp.bfloat16)

    def gather_to(slot, sem, kv):
        return remote(obuf.at[slot], obuf.at[slot], sem, orecv.at[slot], kv, me_tp)

    for step in range(1, nz):
        kv = lax.rem(me_z + step, nz) * ny + me_y
        copy = gather_to(me_kv, osend.at[step], kv)
        copy.start()
        sends.append(copy)
    for step in range(nz):
        slot = lax.rem(me_z + step, nz) * ny + me_y
        if step:
            gather_to(slot, osend.at[step], slot).wait_recv()
        copy = gather_to(slot, fsend.at[step], mate)
        copy.start()
        sends.append(copy)
    for step in range(nz):
        slot = lax.rem(me_z + step, nz) * ny + (1 - me_y)
        gather_to(slot, fsend.at[step], mate).wait_recv()

    half = wout_ref.shape[1] // ntp
    joined = obuf[...].reshape(nkv * each, channels)
    partial_out = jnp.dot(joined, wout_ref[...], preferred_element_type=jnp.float32)
    low, high = partial_out[:, :half], partial_out[:, half:]
    pbuf[...] = jnp.where(me_tp == 0, high, low)
    swap = remote(pbuf, xbuf, xsems.at[0], xsems.at[1], me_kv, other)
    swap.start()
    kept = jnp.where(me_tp == 0, low, high)
    swap.wait()
    mixed = kept + xbuf[...]
    ones = jnp.ones((8, half), jnp.float32)
    local_squares = lax.dot_general(
        ones,
        mixed * mixed,
        (((1,), (1,)), ((), ())),
        precision=lax.Precision.HIGHEST,
        preferred_element_type=jnp.float32,
    )
    mine = me_kv * ntp + me_tp
    nbuf[mine] = local_squares[:1]
    for step in range(1, nkv * ntp):
        kv = lax.rem(me_kv + step // ntp, nkv)
        tp = lax.rem(me_tp + step % ntp, ntp)
        copy = remote(nbuf.at[mine], nbuf.at[mine], nsend.at[step], nrecv.at[mine], kv, tp)
        copy.start()
        sends.append(copy)
    for step in range(1, nkv * ntp):
        kv = lax.rem(me_kv + step // ntp, nkv)
        tp = lax.rem(me_tp + step % ntp, ntp)
        slot = kv * ntp + tp
        remote(
            nbuf.at[slot], nbuf.at[slot], nsend.at[step], nrecv.at[slot], kv, tp
        ).wait_recv()
    norm = nbuf[0]
    for slot in range(1, nkv * ntp):
        norm = norm + nbuf[slot]
    full = half * ntp * nkv
    factor = lax.rsqrt(norm / full + epsilon)
    factor = jnp.broadcast_to(factor, (half, nkv * each)).T
    out_ref[...] = (mixed * factor * gout_ref[...]).astype(jnp.bfloat16)
    for copy in sends:
        copy.wait_send()


def project_output(nkv, heads, values, stats, w_out, gain_out):
    _, each, channels = values.shape
    half = w_out.shape[1] // 2
    rows = nkv * each
    nz = nkv // 2
    vmem = pl.BlockSpec(memory_space=pltpu.VMEM)
    dma = pltpu.SemaphoreType.DMA
    return pl.pallas_call(
        functools.partial(output_kernel, nkv, heads),
        out_shape=jax.ShapeDtypeStruct((rows, half), jnp.bfloat16),
        in_specs=[vmem] * 4,
        out_specs=vmem,
        scratch_shapes=[
            pltpu.VMEM((2 * heads, nz * each), jnp.float32),
            pltpu.VMEM((2 * heads, nz * each), jnp.float32),
            pltpu.VMEM((nz, 2 * heads, nz * each), jnp.float32),
            pltpu.VMEM((2, nz, each, 128), jnp.float32),
            pltpu.VMEM((nz, each, channels), jnp.bfloat16),
            pltpu.VMEM((nz, each, channels), jnp.bfloat16),
            pltpu.VMEM((nz, each, channels), jnp.bfloat16),
            pltpu.VMEM((nkv, each, channels), jnp.bfloat16),
            pltpu.VMEM((rows, half), jnp.float32),
            pltpu.VMEM((rows, half), jnp.float32),
            pltpu.VMEM((nkv * 2, 1, rows), jnp.float32),
            dma((2,)),
            dma((nz,)),
            dma((nz,)),
            dma((nz,)),
            dma((nz,)),
            dma((nz,)),
            dma((nz,)),
            dma((nz,)),
            dma((nkv,)),
            dma((nz,)),
            dma((2,)),
            dma((nkv * 2,)),
            dma((nkv * 2,)),
        ],
        compiler_params=pltpu.CompilerParams(
            collective_id=2, has_side_effects=True, vmem_limit_bytes=48 * 1024 * 1024
        ),
    )(values, stats, w_out, gain_out[None])


def ancestry_fast(parents):
    proposals = parents.shape[-1]
    link = (parents[..., :, None] == jnp.arange(proposals, dtype=jnp.int32)).astype(jnp.bfloat16)
    reaches = link + jnp.eye(proposals, dtype=jnp.bfloat16)
    span = 2
    while span < proposals:
        link = jnp.einsum("sij,sjk->sik", link, link)
        reaches = reaches + jnp.einsum("sij,sjk->sik", reaches, link)
        span *= 2
    reaches = reaches.astype(jnp.float32)
    depths = (jnp.sum(reaches, axis=-1) - 1.0).astype(jnp.int32)
    return (reaches, depths)


def local_plain(
    tokens,
    gain_in,
    w_qdown,
    w_kvdown,
    w_ropek,
    gain_qlat,
    gain_kvlat,
    w_qup,
    gain_q,
    w_ukey,
    w_uval,
    w_out,
    gain_out,
    cache_lat,
    cache_rope,
    parents,
    lengths,
    accepted,
):
    seq_count, proposals, local_width = tokens.shape
    full_width = local_width * lax.axis_size(("kv", "tp"))
    tok_rows = tokens.astype(jnp.float32).reshape(seq_count * proposals, local_width)
    scaled = (tok_rows * gain_in).astype(jnp.bfloat16)
    squares = jnp.sum(tok_rows * tok_rows, axis=-1)
    rope_rows = lax.dynamic_slice_in_dim(
        w_ropek, lax.axis_index(("kv", "tp")) * local_width, local_width, 0
    )
    joined = jnp.concatenate([w_qdown, w_kvdown, rope_rows], axis=1)
    partial_rows = jnp.dot(scaled, joined, preferred_element_type=jnp.float32)
    summed, total_squares = lax.psum((partial_rows, squares), ("kv", "tp"))
    query_latent, new_latent, new_rope = latents(
        summed, total_squares, full_width, gain_qlat, gain_kvlat
    )
    qrank = w_qup.shape[0]
    heads_here = w_qup.shape[1]
    qkhead = w_qup.shape[2]
    kvrank = w_ukey.shape[0]
    nope_dim = w_ukey.shape[2]
    vhead = w_uval.shape[2]
    rope_dim = cache_rope.shape[1]
    half_dim = rope_dim // 2
    reaches, depths = ancestry(parents)
    starts = lengths + accepted
    query_pos = starts[:, None] + depths
    queries = jnp.dot(
        query_latent, w_qup.reshape(qrank, heads_here * qkhead), preferred_element_type=jnp.float32
    )
    queries = normed(queries.reshape(seq_count, proposals, heads_here, qkhead), gain_q)
    query_nope = queries[..., :nope_dim].astype(jnp.bfloat16)
    angles = rope_angles(query_pos, half_dim)[:, :, None, :]
    cosine = jnp.cos(angles)
    sines = jnp.sin(angles)
    lower_half = queries[..., nope_dim : nope_dim + half_dim]
    upper_half = queries[..., nope_dim + half_dim :]
    query_rot = jnp.concatenate(
        [lower_half * cosine - upper_half * sines, upper_half * cosine + lower_half * sines],
        axis=-1,
    ).astype(jnp.bfloat16)
    query_lat = jnp.einsum(
        "sihn,khn->sihk", query_nope, w_ukey, preferred_element_type=jnp.float32
    ).astype(jnp.bfloat16)
    pos_count = cache_lat.shape[1]
    slots = lax.axis_index("kv") * pos_count + jnp.arange(pos_count, dtype=jnp.int32)
    offset = slots[None, :] - starts[:, None]
    inside = (offset >= 0) & (offset < proposals)
    matches = offset[:, :, None] == jnp.arange(proposals, dtype=jnp.int32)
    selector = matches.astype(jnp.bfloat16)
    new_latent = new_latent.reshape(seq_count, proposals, kvrank)
    new_rope = new_rope.reshape(seq_count, proposals, rope_dim)
    placed = jnp.einsum(
        "spj,sjk->spk", selector, new_latent, preferred_element_type=jnp.float32
    ).astype(jnp.bfloat16)
    lat_out = jnp.where(inside[:, :, None], placed, cache_lat)
    placed_rope = jnp.einsum(
        "spj,sjr->srp", selector, new_rope, preferred_element_type=jnp.float32
    ).astype(jnp.bfloat16)
    rope_out = jnp.where(inside[:, None, :], placed_rope, cache_rope)
    key_pos = jnp.where(
        inside,
        starts[:, None] + jnp.sum(jnp.where(matches, depths[:, None, :], 0), axis=-1),
        slots[None, :],
    )
    ancestor = jnp.einsum(
        "sij,spj->sip", reaches, matches.astype(jnp.float32), precision=lax.Precision.HIGHEST
    )
    visible = (offset < 0)[:, None, :] | (ancestor > 0.5)
    key_angles = jnp.swapaxes(rope_angles(key_pos, half_dim), 1, 2)
    key_cos = jnp.cos(key_angles)
    key_sin = jnp.sin(key_angles)
    rope32 = rope_out.astype(jnp.float32)
    key_low = rope32[:, :half_dim, :]
    key_high = rope32[:, half_dim:, :]
    key_rot = jnp.concatenate(
        [key_low * key_cos - key_high * key_sin, key_high * key_cos + key_low * key_sin], axis=1
    ).astype(jnp.bfloat16)
    scores = (
        jnp.einsum("sihk,spk->sihp", query_lat, lat_out, preferred_element_type=jnp.float32)
        + jnp.einsum("sihr,srp->sihp", query_rot, key_rot, preferred_element_type=jnp.float32)
    ) * qkhead ** (-0.5)
    masked = jnp.where(visible[:, :, None, :], scores, -jnp.inf)
    row_max = lax.pmax(jnp.max(masked, axis=-1), "kv")
    weights32 = jnp.exp(masked - row_max[..., None])
    denominator = jnp.sum(weights32, axis=-1)
    weights = weights32.astype(jnp.bfloat16)
    numerator = jnp.einsum("sihp,spk->sihk", weights, lat_out, preferred_element_type=jnp.float32)
    value_map = w_uval.astype(jnp.float32)
    numer_values = apply_values(numerator, value_map)
    values_all, denom_all = lax.psum((numer_values, denominator), "kv")
    head_out = (values_all / denom_all[..., None]).astype(jnp.bfloat16)
    head_rows = head_out.reshape(seq_count * proposals, heads_here * vhead)
    partial_out = jnp.dot(head_rows, w_out, preferred_element_type=jnp.float32).reshape(
        seq_count, proposals, w_out.shape[1]
    )
    mixed = lax.psum_scatter(partial_out, "tp", scatter_dimension=2, tiled=True)
    local_squares = jnp.sum(mixed * mixed, axis=-1)
    norm_total = lax.psum(local_squares, ("kv", "tp"))
    result = (mixed * lax.rsqrt(norm_total / full_width + epsilon)[..., None] * gain_out).astype(
        jnp.bfloat16
    )
    return (result, lat_out, rope_out)


def local_fast(
    tokens,
    gain_in,
    w_qdown,
    w_kvdown,
    w_ropek,
    gain_qlat,
    gain_kvlat,
    w_qup,
    gain_q,
    w_ukey,
    w_uval,
    w_out,
    gain_out,
    cache_lat,
    cache_rope,
    parents,
    lengths,
    accepted,
):
    seq_count, proposals, local_width = tokens.shape
    nkv = lax.axis_size("kv")
    query_latent, new_latent, new_rope = gather_latents(
        nkv,
        tokens.reshape(seq_count * proposals, local_width),
        gain_in,
        w_qdown,
        w_kvdown,
        w_ropek,
        gain_qlat,
        gain_kvlat,
    )
    qrank = w_qup.shape[0]
    heads_here = w_qup.shape[1]
    qkhead = w_qup.shape[2]
    kvrank = w_ukey.shape[0]
    nope_dim = w_ukey.shape[2]
    vhead = w_uval.shape[2]
    rope_dim = cache_rope.shape[1]
    half_dim = rope_dim // 2
    reaches, depths = ancestry_fast(parents)
    starts = lengths + accepted
    query_pos = starts[:, None] + depths
    queries = jnp.dot(
        query_latent, w_qup.reshape(qrank, heads_here * qkhead), preferred_element_type=jnp.float32
    )
    queries = normed(queries.reshape(seq_count, proposals, heads_here, qkhead), gain_q)
    query_nope = queries[..., :nope_dim].astype(jnp.bfloat16)
    angles = rope_angles(query_pos, half_dim)[:, :, None, :]
    cosine = jnp.cos(angles)
    sines = jnp.sin(angles)
    lower_half = queries[..., nope_dim : nope_dim + half_dim]
    upper_half = queries[..., nope_dim + half_dim :]
    query_rot = jnp.concatenate(
        [lower_half * cosine - upper_half * sines, upper_half * cosine + lower_half * sines],
        axis=-1,
    ).astype(jnp.bfloat16)
    query_lat = jnp.einsum(
        "sihn,khn->sihk", query_nope, w_ukey, preferred_element_type=jnp.float32
    ).astype(jnp.bfloat16)
    pos_count = cache_lat.shape[1]
    slots = lax.axis_index("kv") * pos_count + jnp.arange(pos_count, dtype=jnp.int32)
    offset = slots[None, :] - starts[:, None]
    inside = (offset >= 0) & (offset < proposals)
    matches = offset[:, :, None] == jnp.arange(proposals, dtype=jnp.int32)
    selector = matches.astype(jnp.bfloat16)
    new_latent = new_latent.reshape(seq_count, proposals, kvrank)
    new_rope = new_rope.reshape(seq_count, proposals, rope_dim)
    placed = jnp.einsum(
        "spj,sjk->spk", selector, new_latent, preferred_element_type=jnp.float32
    ).astype(jnp.bfloat16)
    lat_out = jnp.where(inside[:, :, None], placed, cache_lat)
    placed_rope = jnp.einsum(
        "spj,sjr->srp", selector, new_rope, preferred_element_type=jnp.float32
    ).astype(jnp.bfloat16)
    rope_out = jnp.where(inside[:, None, :], placed_rope, cache_rope)
    key_pos = jnp.where(
        inside,
        starts[:, None] + jnp.sum(jnp.where(matches, depths[:, None, :], 0), axis=-1),
        slots[None, :],
    )
    ancestor = jnp.einsum(
        "sij,spj->sip", reaches, matches.astype(jnp.float32), precision=lax.Precision.HIGHEST
    )
    visible = (offset < 0)[:, None, :] | (ancestor > 0.5)
    key_angles = jnp.swapaxes(rope_angles(key_pos, half_dim), 1, 2)
    key_cos = jnp.cos(key_angles)
    key_sin = jnp.sin(key_angles)
    rope32 = rope_out.astype(jnp.float32)
    key_low = rope32[:, :half_dim, :]
    key_high = rope32[:, half_dim:, :]
    key_rot = jnp.concatenate(
        [key_low * key_cos - key_high * key_sin, key_high * key_cos + key_low * key_sin], axis=1
    ).astype(jnp.bfloat16)
    scores = (
        jnp.einsum("sihk,spk->sihp", query_lat, lat_out, preferred_element_type=jnp.float32)
        + jnp.einsum("sihr,srp->sihp", query_rot, key_rot, preferred_element_type=jnp.float32)
    ) * qkhead ** (-0.5)
    masked = jnp.where(visible[:, :, None, :], scores, -1e30)
    row_max = jnp.max(masked, axis=-1)
    weights32 = jnp.exp(masked - row_max[..., None])
    denominator = jnp.sum(weights32, axis=-1)
    weights = weights32.astype(jnp.bfloat16)
    numerator = jnp.einsum("sihp,spk->sihk", weights, lat_out, preferred_element_type=jnp.float32)
    numer_values = apply_values(numerator, w_uval.astype(jnp.float32)).astype(jnp.bfloat16)
    each = seq_count * proposals // nkv
    stats = jnp.concatenate([row_max, denominator], axis=-1)
    stats = stats.reshape(nkv // 2, 2, each, 2 * heads_here).transpose(1, 3, 0, 2)
    stats = stats.reshape(2, 2 * heads_here, nkv // 2 * each)
    result = project_output(
        nkv,
        heads_here,
        numer_values.reshape(nkv, each, heads_here * vhead),
        stats,
        w_out,
        gain_out,
    )
    return (result.reshape(seq_count, proposals, local_width), lat_out, rope_out)


def solution(mesh):
    placed = (
        P("dp", None, ("kv", "tp")),
        P(("kv", "tp")),
        P(("kv", "tp"), None),
        P(("kv", "tp"), None),
        P(),
        P(),
        P(),
        P(None, "tp", None),
        P(),
        P(None, "tp", None),
        P(None, "tp", None),
        P("tp", "kv"),
        P(("kv", "tp")),
        P("dp", "kv", None),
        P("dp", None, "kv"),
        P("dp", None),
        P("dp"),
        P("dp"),
    )
    nkv, ntp = mesh.shape["kv"], mesh.shape["tp"]

    def local(*args):
        tokens, w_qup, w_uval = args[0], args[7], args[10]
        rows = tokens.shape[0] * tokens.shape[1]
        fits = ntp == 2 and nkv % 2 == 0 and rows % (16 * nkv * ntp) == 0
        heads = w_qup.shape[1]
        fits = fits and rows % 256 == 0 and (nkv // 2 + 1) * heads <= 128 and heads % 8 == 0
        fits = fits and tokens.shape[2] % 128 == 0 and w_uval.shape[2] % 128 == 0
        return (local_fast if fits else local_plain)(*args)

    return jax.shard_map(
        local,
        mesh=mesh,
        in_specs=placed,
        out_specs=(P("dp", None, ("kv", "tp")), P("dp", "kv", None), P("dp", None, "kv")),
        check_vma=False,
    )
```
